32 devices in a mesh: ep: 8 (over z, core), tp: 4 (over y, x).
Axes of the slice: x: 2, y: 2, z: 4, core: 2. Of those that a mesh axis runs over, the one named last changes fastest.
Arguments:
- tokens: bfloat16 [128, 2048], P('ep'), may hold values from -6 to 6
- old_state: bfloat16 [128, 256, 2048], P('ep', None, 'tp'), may hold values from -3 to 3
- first_gain: bfloat16 [2048], replicated, may hold values from 0.099609375 to 1.8984375
- query_weight: bfloat16 [2048, 1024], P('tp'), may hold values from -0.125 to 0.125
- key_weight: bfloat16 [2048, 1024], P('tp'), may hold values from -0.125 to 0.125
- value_weight: bfloat16 [2048, 2048], P(None, 'tp'), may hold values from -0.125 to 0.125
- outgate_weight: bfloat16 [2048, 2048], P(None, 'tp'), may hold values from -0.125 to 0.125
- lowrank_weight: bfloat16 [2048, 16], replicated, may hold values from -0.125 to 0.125
- decay_weight: bfloat16 [16, 1024], replicated, may hold values from -20 to 20
- decay_bias: float32 [1024], replicated, may hold values from -40 to 2
- head_gain: bfloat16 [2048], P('tp'), may hold values from 0.099609375 to 1.8984375
- output_weight: bfloat16 [2048, 2048], P('tp'), may hold values from -0.125 to 0.125
- second_gain: bfloat16 [2048], replicated, may hold values from 0.099609375 to 1.8984375
- expert_gate: bfloat16 [8, 2048, 1920], P('ep', None, 'tp'), may hold values from -0.125 to 0.125
- expert_up: bfloat16 [8, 2048, 1920], P('ep', None, 'tp'), may hold values from -0.125 to 0.125
- expert_down: bfloat16 [8, 1920, 2048], P('ep', 'tp'), may hold values from -0.125 to 0.125
- shared_gate: bfloat16 [2048, 1920], P(None, 'tp'), may hold values from -0.125 to 0.125
- shared_up: bfloat16 [2048, 1920], P(None, 'tp'), may hold values from -0.125 to 0.125
- shared_down: bfloat16 [1920, 2048], P('tp'), may hold values from -0.125 to 0.125
- route_ids: int32 [128, 4], P('ep'), may hold values from 0 to 7, all different within a row; in each aligned block of 16 rows (0 to 15, 16 to 31, ...) at most 16 rows name the same one
- route_weights: float32 [128, 4], P('ep'), may hold values from 0.1 to 1
Outputs:
- layer_out: bfloat16 [128, 2048], P('ep', 'tp')
- new_state: bfloat16 [128, 256, 2048], P('ep', None, 'tp')
The draws below stay inside these ranges and needn't reach their ends.
Inputs may be any that keep to these rules, and one draw needn't show every extreme that they name: `route_ids`: within the rows of one device (aligned blocks of 16 rows) no expert is named more than 16 times, a bound that some block reaches.
All inputs are finite; a program needn't handle non-finite values.
Results may differ from the reference program's by a relative error of at most 0.035.
Values may be sent and summed in bfloat16 or wider, within the bound.
A program may use at most 64 MiB of HBM per device.

```python
import math
import jax
import jax.numpy as jnp
import numpy as np
from jax import lax

D = 2048
HEADS = 4
DK = 256
DV = 512
RANK = 16
FE = 1920
TOPK = 4
SEQ_DEV = 16
QKW = 1024
VW = 2048
FE_DEV = 480
EXPERTS = 8
CAP = 16
SEQS = 128
N_EP = 8
N_TP = 4


def block_scale(own_key, dims, cuts, least, largest):
    def one(position, parts):
        heights = jax.random.uniform(jax.random.fold_in(jax.random.fold_in(own_key, 6), position), (parts,), jnp.float32, least / len(cuts), largest / len(cuts))
        return jnp.repeat(jnp.exp(heights), dims[position] // parts).reshape((-1,) + (1,) * (len(dims) - position - 1))

    level = one(*cuts[0])
    for cut in cuts[1:]:
        level = level * one(*cut)
    return level


def routed_block(own_key, own, number, rows, amount, top, reach, lean):
    ranking = jax.random.permutation(own_key, amount)
    crowded, ordinary = portions_of(amount, rows * top, reach, lean, True), portions_of(amount, rows * top, reach, lean, False)
    places = jnp.arange(amount)

    def named(tallies, offset_by):
        used = int((tallies > 0).sum())
        fixed = max(1, used // 4)
        shifted = fixed + (places - fixed + offset_by * (used - fixed)) % max(1, amount - fixed)
        return jnp.zeros((amount,), jnp.int32).at[ranking[jnp.where(places < fixed, places, shifted)]].set(jnp.asarray(tallies, jnp.int32))

    tallies = jnp.where(number % 4 == 0, named(crowded, number // 4), named(ordinary, number - number // 4 - 1))
    mixed = jax.random.permutation(jax.random.fold_in(own, 3), amount)
    source_of, receiver = mixed[0:amount // 2 * 2:2], mixed[1:amount // 2 * 2:2]
    room = jnp.minimum(tallies[source_of] - 1, reach - tallies[receiver]) // 2
    room = jnp.where((source_of == ranking[0]) | (receiver == ranking[0]) | (tallies[receiver] == 0), 0, jnp.maximum(room, 0))
    shifted = jax.random.randint(jax.random.fold_in(own, 4), (amount // 2,), 0, 1 << 20) % (room + 1)
    tallies = tallies.at[source_of].add(-shifted).at[receiver].add(shifted)
    members = jnp.searchsorted(jnp.cumsum(tallies), jnp.arange(rows * top), side="right").astype(jnp.int32)
    table = members.reshape(top, rows).T
    table = table[jax.random.permutation(jax.random.fold_in(own, 1), rows)]
    offset_by = jax.random.randint(jax.random.fold_in(own, 2), (rows, 1), 0, top)
    return jnp.take_along_axis(table, (jnp.arange(top)[None, :] + offset_by) % top, axis=1)


def portions_of(number_of, total, reach, skew, full):
    weights = [(1 << 20) // math.isqrt(standing ** skew) + 1 for standing in range(1, number_of + 1)]
    largest = reach if full else min(reach, max(-(-total // number_of), total * weights[0] // sum(weights)))
    least = 1 if total - largest >= number_of - 1 else 0
    holding, surplus = [largest] + [least] * (number_of - 1), total - largest - least * (number_of - 1)
    while surplus > 0:
        free = [i for i in range(1, number_of) if holding[i] < largest] or [i for i in range(1, number_of) if holding[i] < reach]
        mass, remaining = sum([weights[i] for i in free]), surplus
        for i in free:
            more = min(reach - holding[i], max(1, remaining * weights[i] // mass), surplus)
            holding[i] = holding[i] + more
            surplus = surplus - more
    return np.array(holding)


def centred(stream_key, shape, spread, limit, cuts=(), kind=jnp.bfloat16):
    drawn = jax.random.normal(stream_key, shape, jnp.float32) * spread
    if len(cuts) > 0:
        drawn = block_scale(stream_key, shape, cuts, -0.22, 0.18) * drawn
    return jnp.clip(drawn, min=-limit, max=limit).astype(kind)


def setup_inputs(seed: int = 0) -> dict:
    key_of = jax.random.split(jax.random.key(seed), 22)
    tokens = centred(key_of[0], (SEQS, D), 1.0, 6.0, ((0, 8),))
    old_state = centred(key_of[1], (SEQS, DK, VW), 0.5, 3.0, ((0, 8), (2, 4)))
    first_gain = jnp.clip(1.0 + 0.18 * jax.random.normal(key_of[2], (D,), jnp.float32), 0.099609375, 1.8984375).astype(jnp.bfloat16)
    query_weight = centred(key_of[3], (D, QKW), D ** -0.5, 0.125, ((0, 4),))
    key_weight = centred(key_of[4], (D, QKW), D ** -0.5, 0.125, ((0, 4),))
    value_weight = centred(key_of[5], (D, VW), D ** -0.5, 0.125, ((1, 4),))
    outgate_weight = centred(key_of[6], (D, VW), D ** -0.5, 0.125, ((1, 4),))
    lowrank_weight = centred(key_of[7], (D, RANK), D ** -0.5, 0.125)
    decay_weight = centred(key_of[8], (RANK, QKW), 4.0, 20.0)
    decay_bias = jnp.clip(jax.random.uniform(key_of[9], (QKW,), jnp.float32, -40.0, 2.0), -40.0, 2.0)
    head_gain = jnp.clip(1.0 + 0.18 * jax.random.normal(key_of[10], (VW,), jnp.float32), 0.099609375, 1.8984375).astype(jnp.bfloat16)
    output_weight = centred(key_of[11], (VW, D), VW ** -0.5, 0.125, ((0, 4),))
    second_gain = jnp.clip(1.0 + 0.18 * jax.random.normal(key_of[12], (D,), jnp.float32), 0.099609375, 1.8984375).astype(jnp.bfloat16)
    expert_gate = centred(key_of[13], (EXPERTS, D, FE), D ** -0.5, 0.125, ((0, 8), (2, 4)))
    expert_up = centred(key_of[14], (EXPERTS, D, FE), D ** -0.5, 0.125, ((0, 8), (2, 4)))
    expert_down = centred(key_of[15], (EXPERTS, FE, D), FE ** -0.5, 0.125, ((0, 8), (1, 4)))
    shared_gate = centred(key_of[16], (D, FE), D ** -0.5, 0.125, ((1, 4),))
    shared_up = centred(key_of[17], (D, FE), D ** -0.5, 0.125, ((1, 4),))
    shared_down = centred(key_of[18], (FE, D), FE ** -0.5, 0.125, ((0, 4),))
    route_ids_keys = jax.random.split(jax.random.fold_in(key_of[19], 1), SEQS // SEQ_DEV)
    route_ids_turns = jax.random.permutation(jax.random.fold_in(key_of[19], 3), SEQS // SEQ_DEV)
    route_ids = jax.vmap(lambda own, number: routed_block(jax.random.fold_in(key_of[19], 2), own, number, SEQ_DEV, EXPERTS, TOPK, CAP, 2))(route_ids_keys, route_ids_turns).reshape((SEQS, TOPK))
    route_weights = jnp.clip(jnp.exp(math.log(1.0) - 2.3025851 * jax.random.uniform(key_of[20], (SEQS, TOPK), jnp.float32) ** block_scale(key_of[20], (SEQS, TOPK), ((0, 8),), -0.2, 0.2)), 0.1, 1.0)
    return dict(tokens=tokens, old_state=old_state, first_gain=first_gain, query_weight=query_weight, key_weight=key_weight, value_weight=value_weight, outgate_weight=outgate_weight, lowrank_weight=lowrank_weight, decay_weight=decay_weight, decay_bias=decay_bias, head_gain=head_gain, output_weight=output_weight, second_gain=second_gain, expert_gate=expert_gate, expert_up=expert_up, expert_down=expert_down, shared_gate=shared_gate, shared_up=shared_up, shared_down=shared_down, route_ids=route_ids, route_weights=route_weights)


EPSILON = 1e-06

def rms_norm(values, norm_gain):
    floats = values.astype(jnp.float32)
    scaled = floats * lax.rsqrt(lax.optimization_barrier(jnp.mean(floats * floats, axis=-1, keepdims=True)) + EPSILON)
    return (scaled * norm_gain.astype(jnp.float32)).astype(jnp.bfloat16)

def project(left_side, right_side):
    return jnp.dot(left_side, right_side, preferred_element_type=jnp.float32)

def rounded_blocks(hidden, down_matrix):
    row_count = hidden.shape[0]
    pieces = jnp.einsum('rnf,nfd->nrd', hidden.reshape(row_count, N_TP, FE_DEV).astype(jnp.float32), down_matrix.reshape(N_TP, FE_DEV, D).astype(jnp.float32), precision=lax.Precision.HIGHEST)
    pieces = lax.optimization_barrier(pieces.astype(jnp.bfloat16)).astype(jnp.float32)
    return lax.optimization_barrier(jnp.sum(pieces, axis=0))

def reference(tokens, old_state, first_gain, query_weight, key_weight, value_weight, outgate_weight, lowrank_weight, decay_weight, decay_bias, head_gain, output_weight, second_gain, expert_gate, expert_up, expert_down, shared_gate, shared_up, shared_down, route_ids, route_weights):
    seq_count = tokens.shape[0]
    normed = rms_norm(tokens, first_gain)
    query_rows = project(normed, query_weight).astype(jnp.bfloat16)
    key_rows = project(normed, key_weight).astype(jnp.bfloat16)
    value_rows = project(normed, value_weight).astype(jnp.bfloat16)
    out_gate = project(normed, outgate_weight).astype(jnp.bfloat16)
    lowrank = project(normed, lowrank_weight).astype(jnp.bfloat16)
    log_decay = jax.nn.log_sigmoid(project(lowrank, decay_weight) + decay_bias.astype(jnp.float32)) / 16.0
    decay_rows = jnp.exp(log_decay).reshape(seq_count, HEADS, DK).transpose(0, 2, 1)
    key_cols = key_rows.astype(jnp.float32).reshape(seq_count, HEADS, DK).transpose(0, 2, 1)
    value_cols = value_rows.astype(jnp.float32).reshape(seq_count, HEADS, DV)
    carried = decay_rows[:, :, :, None] * old_state.astype(jnp.float32).reshape(seq_count, DK, HEADS, DV) + key_cols[:, :, :, None] * value_cols[:, None, :, :]
    new_state = carried.reshape(seq_count, DK, VW).astype(jnp.bfloat16)
    query_cols = query_rows.astype(jnp.float32).reshape(seq_count, HEADS, DK)
    read_out = jnp.einsum('bhi,bihc->bhc', query_cols, carried, precision=lax.Precision.HIGHEST) * DK ** (-0.5)
    inverse = lax.rsqrt(lax.optimization_barrier(jnp.mean(read_out * read_out, axis=-1)) + EPSILON)
    mixed_rows = (read_out.reshape(seq_count, VW) * head_gain.astype(jnp.float32) * jax.nn.silu(out_gate.astype(jnp.float32))).astype(jnp.bfloat16)
    per_head = jnp.einsum('bhc,hcd->bhd', mixed_rows.reshape(seq_count, HEADS, DV).astype(jnp.float32), output_weight.reshape(HEADS, DV, D).astype(jnp.float32), precision=lax.Precision.HIGHEST)
    attended = lax.optimization_barrier(jnp.sum(per_head * inverse[:, :, None], axis=1))
    second = (tokens.astype(jnp.float32) + attended).astype(jnp.bfloat16)
    normed_two = rms_norm(second, second_gain)
    shared_hidden = (jax.nn.silu(project(normed_two, shared_gate)) * project(normed_two, shared_up)).astype(jnp.bfloat16)
    shared = rounded_blocks(shared_hidden, shared_down)
    group_ids = route_ids.reshape(N_EP, SEQ_DEV * TOPK).astype(jnp.int32)
    onehot = (group_ids[:, :, None] == jnp.arange(EXPERTS, dtype=jnp.int32)[None, None, :]).astype(jnp.int32)
    slot_rank = lax.optimization_barrier(jnp.sum((jnp.cumsum(onehot, axis=1).astype(jnp.int32) - onehot) * onehot, axis=2)).astype(jnp.int32)
    column = (jnp.arange(N_EP, dtype=jnp.int32)[:, None] * CAP + slot_rank).reshape(-1).astype(jnp.int32)
    flat_ids = group_ids.reshape(-1)
    sources = jnp.repeat(normed_two, TOPK, axis=0)
    buffer = jnp.zeros((EXPERTS, N_EP * CAP, D), jnp.bfloat16).at[flat_ids, column].set(sources)

    def expert_fn(operands):
        incoming, gate_matrix, up_matrix, down_matrix = operands
        hidden = (jax.nn.silu(project(incoming, gate_matrix)) * project(incoming, up_matrix)).astype(jnp.bfloat16)
        return rounded_blocks(hidden, down_matrix).astype(jnp.bfloat16)
    results = lax.map(expert_fn, (buffer, expert_gate, expert_up, expert_down))
    picked = results[flat_ids, column].astype(jnp.float32).reshape(seq_count, TOPK, D)
    routed = lax.optimization_barrier(jnp.sum(picked * route_weights.astype(jnp.float32)[:, :, None], axis=1))
    layer_out = (second.astype(jnp.float32) + shared + routed).astype(jnp.bfloat16)
    return (layer_out, new_state)
```

```python
import functools

import jax
import jax.numpy as jnp
from jax import lax
from jax.experimental import pallas as pl
from jax.experimental.pallas import tpu as pltpu
from jax.sharding import PartitionSpec as P

EPSILON = 1e-06
MESH = pl.DeviceIdType.MESH
F32 = jnp.float32
BF16 = jnp.bfloat16


def silu(v):
    return v / (1.0 + jnp.exp(-v))


def norm_rows(floats, gain):
    scale = lax.rsqrt(jnp.mean(floats * floats, axis=-1, keepdims=True) + EPSILON)
    return (floats * scale * gain.astype(F32)).astype(BF16)


def dot(left, right):
    return jnp.dot(left, right, preferred_element_type=F32)


def layer_kernel(
    n_ep, n_tp, heads,
    tokens, first_gain, lowrank_w, decay_w, decay_b, head_gain, second_gain, ids, weights,
    state_h, qw_h, kw_h, vw_h, gw_h, ow_h, eg_h, eu_h, ed_h, sg_h, su_h, sd_h,
    out, new_state_h,
    qw, kw, vw, gw, ow, eg, eu, ed, sg, su, sd, state, load_sem, store_sem,
    normed, qk_part, qk_send, qk_recv, values, row_cols,
    at_send, at_recv, sq_send, sq_recv, second, rows_in, down_send, down_recv,
    sh_send, sh_recv, back_send, back_recv,
    qk_s, qk_r, at_s, at_r, sq_s, sq_r, z_s, z_r, c_s, c_r, dn_s, dn_r, sh_s, sh_r, bk_s, bk_r,
):
    ep = lax.axis_index("ep")
    tp = lax.axis_index("tp")
    zs = n_ep // 2
    z, core = ep // 2, ep % 2
    batch, width = tokens.shape
    key_width, value_count = state.shape[1], state.shape[2]
    feats = width // n_tp
    head_width = value_count * n_tp // heads
    rows = n_ep * batch

    def tp_peer(d):
        return lax.rem(tp + d, n_tp)

    def ep_at(dz, r):
        return lax.rem(z - dz + zs, zs) * 2 + (core if r == 0 else 1 - core)

    def remote(src, dst, ssem, rsem, ep_to, tp_to):
        return pltpu.make_async_remote_copy(
            src_ref=src, dst_ref=dst, send_sem=ssem, recv_sem=rsem,
            device_id=(ep_to, tp_to), device_id_type=MESH,
        )

    barrier = pltpu.get_barrier_semaphore()
    for d in range(1, n_tp):
        pl.semaphore_signal(barrier, inc=1, device_id=(ep, tp_peer(d)), device_id_type=MESH)
    for d in range(1, n_ep):
        pl.semaphore_signal(
            barrier, inc=1, device_id=(lax.rem(ep + d, n_ep), tp), device_id_type=MESH
        )

    sources = [
        (qw_h, qw), (kw_h, kw), (vw_h, vw), (gw_h, gw), (state_h, state), (ow_h, ow),
        (sg_h, sg), (su_h, su), (sd_h, sd), (eg_h.at[0], eg), (eu_h.at[0], eu), (ed_h.at[0], ed),
    ]
    loads = {}
    for i, (src, dst) in enumerate(sources):
        copy = pltpu.make_async_copy(src, dst, load_sem.at[i])
        copy.start()
        loads[id(dst)] = copy

    def arrived(ref):
        loads[id(ref)].wait()

    tok = tokens[...].astype(F32)
    nrm = norm_rows(tok, first_gain[...])
    normed[...] = nrm
    own = normed[:, pl.ds(pl.multiple_of(tp * feats, 128), feats)]
    qk_cols = heads * key_width
    arrived(qw)
    qk_part[:, :qk_cols] = dot(own, qw[...]).astype(BF16)
    arrived(kw)
    qk_part[:, qk_cols:] = dot(own, kw[...]).astype(BF16)

    def qk_block(peer):
        off = pl.multiple_of((peer * value_count // head_width) * key_width, 128)
        return (
            qk_part[:, pl.ds(off, key_width)],
            qk_part[:, pl.ds(pl.multiple_of(qk_cols + off, 128), key_width)],
        )

    pl.semaphore_wait(barrier, n_tp - 1 + n_ep - 1)

    qk_copies = []
    for d in range(1, n_tp):
        peer = tp_peer(d)
        qb, kb = qk_block(peer)
        qk_send[d, :, :key_width] = qb
        qk_send[d, :, key_width:] = kb
        cp = remote(qk_send.at[d], qk_recv.at[d], qk_s.at[d], qk_r.at[d], ep, peer)
        cp.start()
        qk_copies.append(cp)

    offset = pl.multiple_of((tp * value_count // head_width) * key_width, 128)
    lowrank = dot(nrm, lowrank_w[...]).astype(BF16)
    pre = dot(lowrank, decay_w[:, pl.ds(offset, key_width)]) + decay_b[:, pl.ds(offset, key_width)]
    log_decay = (jnp.minimum(pre, 0.0) - jnp.log1p(jnp.exp(-jnp.abs(pre)))) / 16.0
    decay = jnp.exp(log_decay)
    arrived(vw)
    val = dot(nrm, vw[...]).astype(BF16).astype(F32)
    values[...] = val
    arrived(gw)
    gate = dot(nrm, gw[...]).astype(BF16).astype(F32)
    gated = head_gain[...].astype(F32) * silu(gate)

    q_own, k_own = qk_block(tp)
    query = q_own.astype(F32)
    key = k_own.astype(F32)
    for d in range(1, n_tp):
        qk_copies[d - 1].wait_recv()
        query = query + qk_recv[d, :, :key_width].astype(F32)
        key = key + qk_recv[d, :, key_width:].astype(F32)
    query = query.astype(BF16).astype(F32)
    key = key.astype(BF16).astype(F32)

    scaled = query * decay
    high = scaled.astype(BF16)
    low = (scaled - high.astype(F32)).astype(BF16)
    left = jnp.concatenate([high, low], axis=0)
    row_id = lax.broadcasted_iota(jnp.int32, (batch, value_count), 0)
    arrived(state)

    def read_one(b, acc):
        both = dot(left, state[b])
        return jnp.where(row_id == b, both[:batch] + both[batch:], acc)

    acc = lax.fori_loop(0, batch, read_one, jnp.zeros((batch, value_count), F32), unroll=4)
    qk = jnp.sum(query * key, axis=1, keepdims=True)
    read_out = (acc + qk * val) * key_width ** (-0.5)
    squares = jnp.sum(read_out * read_out, axis=1, keepdims=True)
    mixed = (read_out * gated).astype(BF16)

    if value_count != head_width:
        sq_send[...] = jnp.broadcast_to(squares, sq_send.shape)
        sq_copies = []
        for d in range(1, n_tp):
            cp = remote(sq_send, sq_recv.at[d], sq_s.at[d], sq_r.at[d], ep, tp_peer(d))
            cp.start()
            sq_copies.append(cp)
        my_head = tp * value_count // head_width
        for d in range(1, n_tp):
            sq_copies[d - 1].wait_recv()
            src_head = lax.rem(tp - d + n_tp, n_tp) * value_count // head_width
            same = jnp.where(src_head == my_head, 1.0, 0.0).astype(F32)
            squares = squares + same * sq_recv[d][:, :1]
        for cp in sq_copies:
            cp.wait_send()
    inverse = lax.rsqrt(squares / head_width + EPSILON)

    arrived(ow)
    partial = (dot(mixed, ow[...]) * inverse).astype(BF16)
    at_send[...] = partial
    at_copies = []
    for d in range(1, n_tp):
        cp = remote(at_send, at_recv.at[d], at_s.at[d], at_r.at[d], ep, tp_peer(d))
        cp.start()
        at_copies.append(cp)

    stacked = jnp.concatenate([key, decay, jnp.zeros((128 - 2 * batch, key_width), F32)], axis=0)
    row_cols[...] = stacked.T
    lane = lax.broadcasted_iota(jnp.int32, (key_width, 128), 1)
    step = 32

    def update(b, carry):
        cols = row_cols[...]
        key_col = jnp.sum(jnp.where(lane == b, cols, 0.0), axis=1, keepdims=True)
        dec_col = jnp.sum(jnp.where(lane == b + batch, cols, 0.0), axis=1, keepdims=True)
        value_row = values[pl.ds(b, 1), :]
        for i in range(0, key_width, step):
            old = state[b, i : i + step, :].astype(F32)
            new = dec_col[i : i + step] * old + key_col[i : i + step] * value_row
            state[b, i : i + step, :] = new.astype(BF16)
        return carry

    half = batch // 2
    lax.fori_loop(0, half, update, 0)

    total = tok + 0.0
    attended = partial.astype(F32)
    for d in range(1, n_tp):
        at_copies[d - 1].wait_recv()
        attended = attended + at_recv[d].astype(F32)
    sec = (total + attended).astype(BF16)
    second[...] = sec
    nrm2 = norm_rows(sec.astype(F32), second_gain[...])
    rows_in[0] = nrm2

    z_copies = []
    for dz in range(1, zs):
        cp = remote(
            rows_in.at[0], rows_in.at[2 * dz], z_s.at[dz], z_r.at[dz],
            lax.rem(z + dz, zs) * 2 + core, tp,
        )
        cp.start()
        z_copies.append(cp)
    sibling = z * 2 + 1 - core
    c_copies = [remote(rows_in.at[0], rows_in.at[1], c_s.at[0], c_r.at[0], sibling, tp)]
    c_copies[0].start()

    arrived(sg)
    arrived(su)
    hid = (silu(dot(nrm2, sg[...])) * dot(nrm2, su[...])).astype(BF16)
    arrived(sd)
    sh_copies = []
    for d in list(range(1, n_tp)) + [0]:
        peer = tp_peer(d)
        part = dot(hid, sd[:, pl.ds(pl.multiple_of(peer * feats, 128), feats)]).astype(BF16)
        sh_send[d] = part
        if d > 0:
            cp = remote(sh_send.at[d], sh_recv.at[d], sh_s.at[d], sh_r.at[d], ep, peer)
            cp.start()
            sh_copies.append(cp)

    lax.fori_loop(half, batch, update, 0)
    store = pltpu.make_async_copy(state, new_state_h, store_sem)
    store.start()

    for dz in range(1, zs):
        z_copies[dz - 1].wait_recv()
        cp = remote(
            rows_in.at[2 * dz], rows_in.at[2 * dz + 1], c_s.at[dz], c_r.at[dz], sibling, tp
        )
        cp.start()
        c_copies.append(cp)
    arrived(eg)
    arrived(eu)
    arrived(ed)
    for cp in c_copies:
        cp.wait_recv()

    x = rows_in[...].reshape(rows, width)
    hidden = (silu(dot(x, eg[...])) * dot(x, eu[...])).astype(BF16)
    down_copies = []
    for d in list(range(1, n_tp)) + [0]:
        peer = tp_peer(d)
        part = dot(hidden, ed[:, pl.ds(pl.multiple_of(peer * feats, 128), feats)]).astype(BF16)
        down_send[d] = part
        if d > 0:
            cp = remote(down_send.at[d], down_recv.at[d], dn_s.at[d], dn_r.at[d], ep, peer)
            cp.start()
            down_copies.append(cp)
    summed = down_send[0].astype(F32)
    for d in range(1, n_tp):
        down_copies[d - 1].wait_recv()
        summed = summed + down_recv[d].astype(F32)
    back_send[...] = summed.astype(BF16).reshape(n_ep, batch, feats)

    back_copies = []
    for slot in range(1, n_ep):
        dz, r = slot // 2, slot % 2
        cp = remote(
            back_send.at[slot], back_recv.at[slot], bk_s.at[slot], bk_r.at[slot], ep_at(dz, r), tp
        )
        cp.start()
        back_copies.append(cp)

    shared = sh_send[0].astype(F32)
    for d in range(1, n_tp):
        sh_copies[d - 1].wait_recv()
        shared = shared + sh_recv[d].astype(F32)
    result = shared + second[:, pl.ds(pl.multiple_of(tp * feats, 128), feats)].astype(F32)
    id_vals = ids[...]
    w_vals = weights[...]
    for slot in range(n_ep):
        dz, r = slot // 2, slot % 2
        if slot == 0:
            piece = back_send[0]
        else:
            back_copies[slot - 1].wait_recv()
            piece = back_recv[slot]
        expert = lax.rem(z + dz, zs) * 2 + (core if r == 0 else 1 - core)
        share = jnp.sum(jnp.where(id_vals == expert, w_vals, 0.0), axis=1, keepdims=True)
        result = result + share * piece.astype(F32)
    out[...] = result.astype(BF16)

    for cp in qk_copies + at_copies + z_copies + c_copies + sh_copies + down_copies + back_copies:
        cp.wait_send()
    store.wait()


def body(
    n_ep, n_tp,
    tokens, old_state, first_gain, query_weight, key_weight, value_weight, outgate_weight,
    lowrank_weight, decay_weight, decay_bias, head_gain, output_weight, second_gain,
    expert_gate, expert_up, expert_down, shared_gate, shared_up, shared_down,
    route_ids, route_weights,
):
    batch, width = tokens.shape
    key_width, value_count = old_state.shape[1], old_state.shape[2]
    heads = decay_weight.shape[1] // key_width
    feats = width // n_tp
    qk_cols = heads * key_width
    rows = n_ep * batch
    zs = n_ep // 2
    vmem = pl.BlockSpec(memory_space=pltpu.VMEM)
    hbm = pl.BlockSpec(memory_space=pl.ANY)
    dma = pltpu.SemaphoreType.DMA
    big = [
        query_weight, key_weight, value_weight, outgate_weight, output_weight,
        expert_gate[0], expert_up[0], expert_down[0], shared_gate, shared_up, shared_down,
    ]
    scratch = [pltpu.VMEM(w.shape, BF16) for w in big]
    scratch += [
        pltpu.VMEM(old_state.shape, BF16),
        dma((12,)),
        dma,
        pltpu.VMEM((batch, width), BF16),
        pltpu.VMEM((batch, 2 * qk_cols), BF16),
        pltpu.VMEM((n_tp, batch, 2 * key_width), BF16),
        pltpu.VMEM((n_tp, batch, 2 * key_width), BF16),
        pltpu.VMEM((batch, value_count), F32),
        pltpu.VMEM((key_width, 128), F32),
        pltpu.VMEM((batch, width), BF16),
        pltpu.VMEM((n_tp, batch, width), BF16),
        pltpu.VMEM((batch, 128), F32),
        pltpu.VMEM((n_tp, batch, 128), F32),
        pltpu.VMEM((batch, width), BF16),
        pltpu.VMEM((n_ep, batch, width), BF16),
        pltpu.VMEM((n_tp, rows, feats), BF16),
        pltpu.VMEM((n_tp, rows, feats), BF16),
        pltpu.VMEM((n_tp, batch, feats), BF16),
        pltpu.VMEM((n_tp, batch, feats), BF16),
        pltpu.VMEM((n_ep, batch, feats), BF16),
        pltpu.VMEM((n_ep, batch, feats), BF16),
    ]
    for count in (n_tp, n_tp, n_tp, zs, zs, n_tp, n_tp, n_ep):
        scratch += [dma((count,)), dma((count,))]
    layer_out, new_state = pl.pallas_call(
        functools.partial(layer_kernel, n_ep, n_tp, heads),
        out_shape=(
            jax.ShapeDtypeStruct((batch, feats), BF16),
            jax.ShapeDtypeStruct(old_state.shape, BF16),
        ),
        in_specs=[vmem] * 9 + [hbm] * 12,
        out_specs=(vmem, hbm),
        scratch_shapes=scratch,
        compiler_params=pltpu.CompilerParams(
            collective_id=0, has_side_effects=True, vmem_limit_bytes=60 * 1024 * 1024
        ),
    )(
        tokens, first_gain[None], lowrank_weight, decay_weight, decay_bias[None],
        head_gain[None], second_gain[None], route_ids, route_weights,
        old_state, query_weight, key_weight, value_weight, outgate_weight, output_weight,
        expert_gate, expert_up, expert_down, shared_gate, shared_up, shared_down,
    )
    return layer_out, new_state


def solution(mesh):
    placed = (
        P("ep", None),
        P("ep", None, "tp"),
        P(),
        P("tp", None),
        P("tp", None),
        P(None, "tp"),
        P(None, "tp"),
        P(),
        P(),
        P(),
        P("tp"),
        P("tp", None),
        P(),
        P("ep", None, "tp"),
        P("ep", None, "tp"),
        P("ep", "tp", None),
        P(None, "tp"),
        P(None, "tp"),
        P("tp", None),
        P("ep", None),
        P("ep", None),
    )
    return jax.shard_map(
        functools.partial(body, mesh.shape["ep"], mesh.shape["tp"]),
        mesh=mesh,
        in_specs=placed,
        out_specs=(P("ep", "tp"), P("ep", None, "tp")),
        check_vma=False,
    )
```

```python
import functools

import jax
import jax.numpy as jnp
from jax import lax
from jax.experimental import pallas as pl
from jax.experimental.pallas import tpu as pltpu
from jax.sharding import PartitionSpec as P

EPSILON = 1e-06
MESH = pl.DeviceIdType.MESH
F32 = jnp.float32
BF16 = jnp.bfloat16


def silu(v):
    return v / (1.0 + jnp.exp(-v))


def norm_rows(floats, gain):
    scale = lax.rsqrt(jnp.mean(floats * floats, axis=-1, keepdims=True) + EPSILON)
    return (floats * scale * gain).astype(BF16)


def dot(left, right):
    return jnp.dot(left, right, preferred_element_type=F32)


def dot_t(left, right):
    return lax.dot_general(left, right, (((1,), (1,)), ((), ())), preferred_element_type=F32)


def gain_row(gain_ref):
    gain = gain_ref[...].astype(F32)
    return jnp.concatenate([gain[i : i + 1, :] for i in range(gain.shape[0])], axis=1)


def layer_kernel(
    n_ep, n_tp, heads,
    tokens, first_gain, lowrank_w, decay_w, decay_b, head_gain, second_gain, ids, weights,
    state_h, qw_h, kw_h, vw_h, gw_h, ow_h, eg_h, eu_h, ed_h, sg_h, su_h, sd_h,
    out, state,
    qw, kw, vw, gw, ow, eg, eu, ed, sg, su, sd, load_sem, share_t,
    normed, qk_part, qk_send, qk_recv, values, row_cols,
    at_send, at_recv, sq_send, sq_recv, second, rows_in, down_send, down_recv,
    sh_send, sh_recv, back_send, back_recv,
    qk_s, qk_r, at_s, at_r, sq_s, sq_r, z_s, z_r, c_s, c_r, dn_s, dn_r, sh_s, sh_r, bk_s, bk_r,
):
    ep = lax.axis_index("ep")
    tp = lax.axis_index("tp")
    zs = n_ep // 2
    z, core = ep // 2, ep % 2
    batch, width = tokens.shape
    key_width, value_count = state.shape[1], state.shape[2]
    feats = width // n_tp
    head_width = value_count * n_tp // heads
    rows = n_ep * batch

    def tp_peer(d):
        return lax.rem(tp + d, n_tp)

    def ep_at(dz, r):
        return lax.rem(z - dz + zs, zs) * 2 + (core if r == 0 else 1 - core)

    def remote(src, dst, ssem, rsem, ep_to, tp_to):
        return pltpu.make_async_remote_copy(
            src_ref=src, dst_ref=dst, send_sem=ssem, recv_sem=rsem,
            device_id=(ep_to, tp_to), device_id_type=MESH,
        )

    barrier = pltpu.get_barrier_semaphore()
    for d in range(1, n_tp):
        pl.semaphore_signal(barrier, inc=1, device_id=(ep, tp_peer(d)), device_id_type=MESH)
    for d in range(1, n_ep):
        pl.semaphore_signal(
            barrier, inc=1, device_id=(lax.rem(ep + d, n_ep), tp), device_id_type=MESH
        )

    sources = [
        (qw_h, qw), (kw_h, kw), (vw_h, vw), (gw_h, gw), (state_h, state), (ow_h, ow),
        (sg_h, sg), (su_h, su), (sd_h, sd), (eg_h.at[0], eg), (eu_h.at[0], eu), (ed_h.at[0], ed),
    ]
    loads = {
        id(dst): pltpu.make_async_copy(src, dst, load_sem.at[i])
        for i, (src, dst) in enumerate(sources)
    }
    for src, dst in sources[:5]:
        loads[id(dst)].start()

    def arrived(ref):
        loads[id(ref)].wait()

    tok = tokens[...].astype(F32)
    nrm = norm_rows(tok, gain_row(first_gain))
    normed[...] = nrm
    own = normed[:, pl.ds(pl.multiple_of(tp * feats, 128), feats)]
    qk_cols = heads * key_width
    arrived(qw)
    qk_part[:, :qk_cols] = dot(own, qw[...]).astype(BF16)
    arrived(kw)
    qk_part[:, qk_cols:] = dot(own, kw[...]).astype(BF16)

    def qk_block(peer):
        off = pl.multiple_of((peer * value_count // head_width) * key_width, 128)
        return (
            qk_part[:, pl.ds(off, key_width)],
            qk_part[:, pl.ds(pl.multiple_of(qk_cols + off, 128), key_width)],
        )

    pl.semaphore_wait(barrier, n_tp - 1 + n_ep - 1)

    qk_copies = []
    for d in range(1, n_tp):
        peer = tp_peer(d)
        qb, kb = qk_block(peer)
        qk_send[d, :, :key_width] = qb
        qk_send[d, :, key_width:] = kb
        cp = remote(qk_send.at[d], qk_recv.at[d], qk_s.at[d], qk_r.at[d], ep, peer)
        cp.start()
        qk_copies.append(cp)

    for src, dst in sources[5:]:
        loads[id(dst)].start()

    offset = pl.multiple_of((tp * value_count // head_width) * key_width, 128)
    lowrank = dot_t(nrm, lowrank_w[...]).astype(BF16)
    pre = dot(lowrank, decay_w[:, pl.ds(offset, key_width)]) + decay_b[:, pl.ds(offset, key_width)]
    log_decay = (jnp.minimum(pre, 0.0) - jnp.log1p(jnp.exp(-jnp.abs(pre)))) / 16.0
    decay = jnp.exp(log_decay)
    arrived(vw)
    val = dot(nrm, vw[...]).astype(BF16).astype(F32)
    values[...] = val
    arrived(gw)
    gate = dot(nrm, gw[...]).astype(BF16).astype(F32)
    gated = gain_row(head_gain) * silu(gate)

    q_own, k_own = qk_block(tp)
    query = q_own.astype(F32)
    key = k_own.astype(F32)
    for d in range(1, n_tp):
        qk_copies[d - 1].wait_recv()
        query = query + qk_recv[d, :, :key_width].astype(F32)
        key = key + qk_recv[d, :, key_width:].astype(F32)
    query = query.astype(BF16).astype(F32)
    key = key.astype(BF16).astype(F32)

    scaled = query * decay
    high = scaled.astype(BF16)
    low = (scaled - high.astype(F32)).astype(BF16)
    left = jnp.concatenate([high, low], axis=0)
    row_id = lax.broadcasted_iota(jnp.int32, (batch, value_count), 0)
    arrived(state)

    def read_one(b, acc):
        both = dot(left, state[b])
        return jnp.where(row_id == b, both[:batch] + both[batch:], acc)

    acc = lax.fori_loop(0, batch, read_one, jnp.zeros((batch, value_count), F32), unroll=4)
    qk = jnp.sum(query * key, axis=1, keepdims=True)
    read_out = (acc + qk * val) * key_width ** (-0.5)
    squares = jnp.sum(read_out * read_out, axis=1, keepdims=True)
    mixed = (read_out * gated).astype(BF16)

    if value_count != head_width:
        sq_send[...] = jnp.broadcast_to(squares, sq_send.shape)
        sq_copies = []
        for d in range(1, n_tp):
            cp = remote(sq_send, sq_recv.at[d], sq_s.at[d], sq_r.at[d], ep, tp_peer(d))
            cp.start()
            sq_copies.append(cp)
        my_head = tp * value_count // head_width
        for d in range(1, n_tp):
            sq_copies[d - 1].wait_recv()
            src_head = lax.rem(tp - d + n_tp, n_tp) * value_count // head_width
            same = jnp.where(src_head == my_head, 1.0, 0.0).astype(F32)
            squares = squares + same * sq_recv[d][:, :1]
        for cp in sq_copies:
            cp.wait_send()
    inverse = lax.rsqrt(squares / head_width + EPSILON)

    arrived(ow)
    partial = (dot(mixed, ow[...]) * inverse).astype(BF16)
    at_send[...] = partial
    at_copies = []
    for d in range(1, n_tp):
        cp = remote(at_send, at_recv.at[d], at_s.at[d], at_r.at[d], ep, tp_peer(d))
        cp.start()
        at_copies.append(cp)

    stacked = jnp.concatenate([key, decay, jnp.zeros((128 - 2 * batch, key_width), F32)], axis=0)
    row_cols[...] = stacked.T
    lane = lax.broadcasted_iota(jnp.int32, (key_width, 128), 1)
    step = 32

    def update(b, carry):
        cols = row_cols[...]
        key_col = jnp.sum(jnp.where(lane == b, cols, 0.0), axis=1, keepdims=True)
        dec_col = jnp.sum(jnp.where(lane == b + batch, cols, 0.0), axis=1, keepdims=True)
        value_row = values[pl.ds(b, 1), :]
        for i in range(0, key_width, step):
            old = state[b, i : i + step, :].astype(F32)
            new = dec_col[i : i + step] * old + key_col[i : i + step] * value_row
            state[b, i : i + step, :] = new.astype(BF16)
        return carry

    half = batch // 2
    lax.fori_loop(0, half, update, 0)

    total = tok + 0.0
    attended = partial.astype(F32)
    for d in range(1, n_tp):
        at_copies[d - 1].wait_recv()
        attended = attended + at_recv[d].astype(F32)
    sec = (total + attended).astype(BF16)
    second[...] = sec
    nrm2 = norm_rows(sec.astype(F32), gain_row(second_gain))
    rows_in[0] = nrm2

    z_copies = []
    for dz in range(1, zs):
        cp = remote(
            rows_in.at[0], rows_in.at[2 * dz], z_s.at[dz], z_r.at[dz],
            lax.rem(z + dz, zs) * 2 + core, tp,
        )
        cp.start()
        z_copies.append(cp)
    sibling = z * 2 + 1 - core
    c_copies = [remote(rows_in.at[0], rows_in.at[1], c_s.at[0], c_r.at[0], sibling, tp)]
    c_copies[0].start()

    arrived(sg)
    arrived(su)
    hid = (silu(dot_t(nrm2, sg[...])) * dot_t(nrm2, su[...])).astype(BF16)
    arrived(sd)
    sh_copies = []
    for d in list(range(1, n_tp)) + [0]:
        peer = tp_peer(d)
        part = dot(hid, sd[:, pl.ds(pl.multiple_of(peer * feats, 128), feats)]).astype(BF16)
        sh_send[d] = part
        if d > 0:
            cp = remote(sh_send.at[d], sh_recv.at[d], sh_s.at[d], sh_r.at[d], ep, peer)
            cp.start()
            sh_copies.append(cp)

    lax.fori_loop(half, batch, update, 0)

    for dz in range(1, zs):
        z_copies[dz - 1].wait_recv()
        cp = remote(
            rows_in.at[2 * dz], rows_in.at[2 * dz + 1], c_s.at[dz], c_r.at[dz], sibling, tp
        )
        cp.start()
        c_copies.append(cp)
    arrived(eg)
    arrived(eu)
    arrived(ed)
    for cp in c_copies:
        cp.wait_recv()

    x = rows_in[...].reshape(rows, width)
    hidden = (silu(dot_t(x, eg[...])) * dot_t(x, eu[...])).astype(BF16)
    down_copies = []
    for d in list(range(1, n_tp)) + [0]:
        peer = tp_peer(d)
        part = dot(hidden, ed[:, pl.ds(pl.multiple_of(peer * feats, 128), feats)]).astype(BF16)
        down_send[d] = part
        if d > 0:
            cp = remote(down_send.at[d], down_recv.at[d], dn_s.at[d], dn_r.at[d], ep, peer)
            cp.start()
            down_copies.append(cp)
    summed = down_send[0].astype(F32)
    for d in range(1, n_tp):
        down_copies[d - 1].wait_recv()
        summed = summed + down_recv[d].astype(F32)
    back_send[...] = summed.astype(BF16).reshape(n_ep, batch, feats)

    back_copies = []
    for slot in range(1, n_ep):
        dz, r = slot // 2, slot % 2
        cp = remote(
            back_send.at[slot], back_recv.at[slot], bk_s.at[slot], bk_r.at[slot], ep_at(dz, r), tp
        )
        cp.start()
        back_copies.append(cp)

    shared = sh_send[0].astype(F32)
    for d in range(1, n_tp):
        sh_copies[d - 1].wait_recv()
        shared = shared + sh_recv[d].astype(F32)
    result = shared + second[:, pl.ds(pl.multiple_of(tp * feats, 128), feats)].astype(F32)
    number = lax.broadcasted_iota(jnp.int32, (128, batch), 0)
    table = jnp.zeros((128, batch), F32)
    for k in range(ids.shape[0]):
        table = table + jnp.where(number == ids[k : k + 1, :], weights[k : k + 1, :], 0.0)
    share_t[...] = jnp.zeros_like(share_t)
    share_t[:, :batch] = table
    shares = share_t[...].T[:batch]
    expert_id = lax.broadcasted_iota(jnp.int32, (batch, 128), 1)
    for slot in range(n_ep):
        dz, r = slot // 2, slot % 2
        if slot == 0:
            piece = back_send[0]
        else:
            back_copies[slot - 1].wait_recv()
            piece = back_recv[slot]
        expert = lax.rem(z + dz, zs) * 2 + (core if r == 0 else 1 - core)
        share = jnp.sum(jnp.where(expert_id == expert, shares, 0.0), axis=1, keepdims=True)
        result = result + share * piece.astype(F32)
    out[...] = result.astype(BF16)

    for cp in qk_copies + at_copies + z_copies + c_copies + sh_copies + down_copies + back_copies:
        cp.wait_send()


def body(
    n_ep, n_tp,
    tokens, old_state, first_gain, query_weight, key_weight, value_weight, outgate_weight,
    lowrank_weight, decay_weight, decay_bias, head_gain, output_weight, second_gain,
    expert_gate, expert_up, expert_down, shared_gate, shared_up, shared_down,
    route_ids, route_weights,
):
    batch, width = tokens.shape
    key_width, value_count = old_state.shape[1], old_state.shape[2]
    heads = decay_weight.shape[1] // key_width
    feats = width // n_tp
    qk_cols = heads * key_width
    rows = n_ep * batch
    zs = n_ep // 2
    vmem = pl.BlockSpec(memory_space=pltpu.VMEM)
    hbm = pl.BlockSpec(memory_space=pltpu.HBM)
    dma = pltpu.SemaphoreType.DMA
    big = [
        query_weight, key_weight, value_weight, outgate_weight, output_weight,
        expert_gate[0].T, expert_up[0].T, expert_down[0], shared_gate.T, shared_up.T, shared_down,
    ]
    scratch = [pltpu.VMEM(w.shape, BF16) for w in big]
    scratch += [
        dma((12,)),
        pltpu.VMEM((128, 128), F32),
        pltpu.VMEM((batch, width), BF16),
        pltpu.VMEM((batch, 2 * qk_cols), BF16),
        pltpu.VMEM((n_tp, batch, 2 * key_width), BF16),
        pltpu.VMEM((n_tp, batch, 2 * key_width), BF16),
        pltpu.VMEM((batch, value_count), F32),
        pltpu.VMEM((key_width, 128), F32),
        pltpu.VMEM((batch, width), BF16),
        pltpu.VMEM((n_tp, batch, width), BF16),
        pltpu.VMEM((batch, 128), F32),
        pltpu.VMEM((n_tp, batch, 128), F32),
        pltpu.VMEM((batch, width), BF16),
        pltpu.VMEM((n_ep, batch, width), BF16),
        pltpu.VMEM((n_tp, rows, feats), BF16),
        pltpu.VMEM((n_tp, rows, feats), BF16),
        pltpu.VMEM((n_tp, batch, feats), BF16),
        pltpu.VMEM((n_tp, batch, feats), BF16),
        pltpu.VMEM((n_ep, batch, feats), BF16),
        pltpu.VMEM((n_ep, batch, feats), BF16),
    ]
    for count in (n_tp, n_tp, n_tp, zs, zs, n_tp, n_tp, n_ep):
        scratch += [dma((count,)), dma((count,))]
    layer_out, new_state = pl.pallas_call(
        functools.partial(layer_kernel, n_ep, n_tp, heads),
        out_shape=(
            jax.ShapeDtypeStruct((batch, feats), BF16),
            pltpu.VMEM(old_state.shape, BF16),
        ),
        in_specs=[vmem] * 9 + [hbm] * 12,
        out_specs=(vmem, vmem),
        scratch_shapes=scratch,
        compiler_params=pltpu.CompilerParams(
            collective_id=0, has_side_effects=True, vmem_limit_bytes=57 * 1024 * 1024
        ),
    )(
        tokens, first_gain.reshape(-1, 128), lowrank_weight.T, decay_weight, decay_bias[None],
        head_gain.reshape(-1, 128), second_gain.reshape(-1, 128), route_ids.T, route_weights.T,
        old_state, query_weight, key_weight, value_weight, outgate_weight, output_weight,
        expert_gate.swapaxes(1, 2), expert_up.swapaxes(1, 2), expert_down,
        shared_gate.T, shared_up.T, shared_down,
    )
    return layer_out, new_state


def solution(mesh):
    placed = (
        P("ep", None),
        P("ep", None, "tp"),
        P(),
        P("tp", None),
        P("tp", None),
        P(None, "tp"),
        P(None, "tp"),
        P(),
        P(),
        P(),
        P("tp"),
        P("tp", None),
        P(),
        P("ep", None, "tp"),
        P("ep", None, "tp"),
        P("ep", "tp", None),
        P(None, "tp"),
        P(None, "tp"),
        P("tp", None),
        P("ep", None),
        P("ep", None),
    )
    return jax.shard_map(
        functools.partial(body, mesh.shape["ep"], mesh.shape["tp"]),
        mesh=mesh,
        in_specs=placed,
        out_specs=(P("ep", "tp"), P("ep", None, "tp")),
        check_vma=False,
    )
```

```python
import functools

import jax
import jax.numpy as jnp
from jax import lax
from jax.experimental import pallas as pl
from jax.experimental.pallas import tpu as pltpu
from jax.sharding import PartitionSpec as P

EPSILON = 1e-06
MESH = pl.DeviceIdType.MESH
F32 = jnp.float32
BF16 = jnp.bfloat16


def silu(v):
    return v / (1.0 + jnp.exp(-v))


def norm_rows(floats, gain):
    scale = lax.rsqrt(jnp.mean(floats * floats, axis=-1, keepdims=True) + EPSILON)
    return (floats * scale * gain).astype(BF16)


def dot(left, right):
    return jnp.dot(left, right, preferred_element_type=F32)


def dot_t(left, right):
    return lax.dot_general(left, right, (((1,), (1,)), ((), ())), preferred_element_type=F32)


def gain_row(gain_ref):
    gain = gain_ref[...].astype(F32)
    return jnp.concatenate([gain[i : i + 1, :] for i in range(gain.shape[0])], axis=1)


def layer_kernel(
    n_ep, n_tp, heads,
    tokens, first_gain, lowrank_w, decay_w, decay_b, head_gain, second_gain, ids, weights,
    state_h, qw_h, kw_h, vw_h, gw_h, ow_h, eg_h, eu_h, ed_h, sg_h, su_h, sd_h,
    out, state,
    qw, kw, vw, gw, ow, eg, eu, ed, sg, su, sd, load_sem, share_t,
    normed, qk_part, qk_send, qk_recv, values, row_cols,
    at_send, at_recv, sq_send, sq_recv, second, rows_in, kept, comb_send, comb_recv, down_send, down_recv,
    sh_send, sh_recv, back_send, back_recv,
    qk_s, qk_r, at_s, at_r, sq_s, sq_r, z_s, z_r, c_s, c_r, cb_s, cb_r, dn_s, dn_r, sh_s, sh_r, bk_s, bk_r,
):
    ep = lax.axis_index("ep")
    tp = lax.axis_index("tp")
    zs = n_ep // 2
    z, core = ep // 2, ep % 2
    batch, width = tokens.shape
    key_width, value_count = state.shape[1], state.shape[2]
    feats = width // n_tp
    head_width = value_count * n_tp // heads
    chunks = down_send.shape[0]
    span = zs // chunks

    def tp_peer(d):
        return lax.rem(tp + d, n_tp)

    def along_z(dz):
        return lax.rem(z + dz + zs, zs) * 2 + core

    sibling = z * 2 + 1 - core

    def remote(src, dst, ssem, rsem, ep_to, tp_to):
        return pltpu.make_async_remote_copy(
            src_ref=src, dst_ref=dst, send_sem=ssem, recv_sem=rsem,
            device_id=(ep_to, tp_to), device_id_type=MESH,
        )

    barrier = pltpu.get_barrier_semaphore()
    for d in range(1, n_tp):
        pl.semaphore_signal(barrier, inc=1, device_id=(ep, tp_peer(d)), device_id_type=MESH)
    for dz in range(1, zs):
        pl.semaphore_signal(barrier, inc=1, device_id=(along_z(dz), tp), device_id_type=MESH)
    pl.semaphore_signal(barrier, inc=1, device_id=(sibling, tp), device_id_type=MESH)

    sources = [
        (qw_h, qw), (kw_h, kw), (vw_h, vw), (gw_h, gw), (state_h, state), (ow_h, ow),
        (sg_h, sg), (su_h, su), (sd_h, sd), (eg_h.at[0], eg), (eu_h.at[0], eu), (ed_h.at[0], ed),
    ]
    loads = {
        id(dst): pltpu.make_async_copy(src, dst, load_sem.at[i])
        for i, (src, dst) in enumerate(sources)
    }
    for src, dst in sources[:5]:
        loads[id(dst)].start()

    def arrived(ref):
        loads[id(ref)].wait()

    tok = tokens[...].astype(F32)
    nrm = norm_rows(tok, gain_row(first_gain))
    normed[...] = nrm
    own = normed[:, pl.ds(pl.multiple_of(tp * feats, 128), feats)]
    qk_cols = heads * key_width
    arrived(qw)
    qk_part[:, :qk_cols] = dot(own, qw[...]).astype(BF16)
    arrived(kw)
    qk_part[:, qk_cols:] = dot(own, kw[...]).astype(BF16)

    def qk_block(peer):
        off = pl.multiple_of((peer * value_count // head_width) * key_width, 128)
        return (
            qk_part[:, pl.ds(off, key_width)],
            qk_part[:, pl.ds(pl.multiple_of(qk_cols + off, 128), key_width)],
        )

    pl.semaphore_wait(barrier, n_tp - 1 + zs)

    qk_copies = []
    for d in range(1, n_tp):
        peer = tp_peer(d)
        qb, kb = qk_block(peer)
        qk_send[d, :, :key_width] = qb
        qk_send[d, :, key_width:] = kb
        cp = remote(qk_send.at[d], qk_recv.at[d], qk_s.at[d], qk_r.at[d], ep, peer)
        cp.start()
        qk_copies.append(cp)

    for src, dst in sources[5:]:
        loads[id(dst)].start()

    number = lax.broadcasted_iota(jnp.int32, (128, batch), 0)
    table = jnp.zeros((128, batch), F32)
    for k in range(ids.shape[0]):
        table = table + jnp.where(number == ids[k : k + 1, :], weights[k : k + 1, :], 0.0)
    part_high = table.astype(BF16).astype(F32)
    share_t[...] = jnp.zeros_like(share_t)
    share_t[:n_ep, :batch] = part_high[:n_ep]
    share_t[n_ep : 2 * n_ep, :batch] = (table - part_high)[:n_ep]
    rows_in[0, 0, :, width:] = share_t[...].T[:batch].astype(BF16)

    offset = pl.multiple_of((tp * value_count // head_width) * key_width, 128)
    lowrank = dot_t(nrm, lowrank_w[...]).astype(BF16)
    pre = dot(lowrank, decay_w[:, pl.ds(offset, key_width)]) + decay_b[:, pl.ds(offset, key_width)]
    log_decay = (jnp.minimum(pre, 0.0) - jnp.log1p(jnp.exp(-jnp.abs(pre)))) / 16.0
    decay = jnp.exp(log_decay)
    arrived(vw)
    val = dot(nrm, vw[...]).astype(BF16).astype(F32)
    values[...] = val
    arrived(gw)
    gate = dot(nrm, gw[...]).astype(BF16).astype(F32)
    gated = gain_row(head_gain) * silu(gate)

    q_own, k_own = qk_block(tp)
    query = q_own.astype(F32)
    key = k_own.astype(F32)
    for d in range(1, n_tp):
        qk_copies[d - 1].wait_recv()
        query = query + qk_recv[d, :, :key_width].astype(F32)
        key = key + qk_recv[d, :, key_width:].astype(F32)
    query = query.astype(BF16).astype(F32)
    key = key.astype(BF16).astype(F32)

    scaled = query * decay
    high = scaled.astype(BF16)
    low = (scaled - high.astype(F32)).astype(BF16)
    left = jnp.concatenate([high, low], axis=0)
    row_id = lax.broadcasted_iota(jnp.int32, (batch, value_count), 0)
    arrived(state)

    def read_one(b, acc):
        both = dot(left, state[b])
        return jnp.where(row_id == b, both[:batch] + both[batch:], acc)

    acc = lax.fori_loop(0, batch, read_one, jnp.zeros((batch, value_count), F32), unroll=4)
    qk = jnp.sum(query * key, axis=1, keepdims=True)
    read_out = (acc + qk * val) * key_width ** (-0.5)
    squares = jnp.sum(read_out * read_out, axis=1, keepdims=True)
    mixed = (read_out * gated).astype(BF16)

    if value_count != head_width:
        sq_send[...] = jnp.broadcast_to(squares, sq_send.shape)
        sq_copies = []
        for d in range(1, n_tp):
            cp = remote(sq_send, sq_recv.at[d], sq_s.at[d], sq_r.at[d], ep, tp_peer(d))
            cp.start()
            sq_copies.append(cp)
        my_head = tp * value_count // head_width
        for d in range(1, n_tp):
            sq_copies[d - 1].wait_recv()
            src_head = lax.rem(tp - d + n_tp, n_tp) * value_count // head_width
            same = jnp.where(src_head == my_head, 1.0, 0.0).astype(F32)
            squares = squares + same * sq_recv[d][:, :1]
        for cp in sq_copies:
            cp.wait_send()
    inverse = lax.rsqrt(squares / head_width + EPSILON)

    arrived(ow)
    partial = (dot(mixed, ow[...]) * inverse).astype(BF16)
    at_send[...] = partial
    at_copies = []
    for d in range(1, n_tp):
        cp = remote(at_send, at_recv.at[d], at_s.at[d], at_r.at[d], ep, tp_peer(d))
        cp.start()
        at_copies.append(cp)

    stacked = jnp.concatenate([key, decay, jnp.zeros((128 - 2 * batch, key_width), F32)], axis=0)
    row_cols[...] = stacked.T
    lane = lax.broadcasted_iota(jnp.int32, (key_width, 128), 1)
    step = 32

    def update(b, carry):
        cols = row_cols[...]
        key_col = jnp.sum(jnp.where(lane == b, cols, 0.0), axis=1, keepdims=True)
        dec_col = jnp.sum(jnp.where(lane == b + batch, cols, 0.0), axis=1, keepdims=True)
        value_row = values[pl.ds(b, 1), :]
        for i in range(0, key_width, step):
            old = state[b, i : i + step, :].astype(F32)
            new = dec_col[i : i + step] * old + key_col[i : i + step] * value_row
            state[b, i : i + step, :] = new.astype(BF16)
        return carry

    half = batch // 2
    lax.fori_loop(0, half, update, 0)

    total = tok + 0.0
    attended = partial.astype(F32)
    for d in range(1, n_tp):
        at_copies[d - 1].wait_recv()
        attended = attended + at_recv[d].astype(F32)
    sec = (total + attended).astype(BF16)
    second[...] = sec
    nrm2 = norm_rows(sec.astype(F32), gain_row(second_gain))
    rows_in[0, 0, :, :width] = nrm2

    z_copies = []
    for dz in range(1, zs):
        cp = remote(
            rows_in.at[0, 0], rows_in.at[0, dz], z_s.at[dz], z_r.at[dz], along_z(dz), tp
        )
        cp.start()
        z_copies.append(cp)
    c_copies = []

    def forward(dz):
        if dz > 0:
            z_copies[dz - 1].wait_recv()
        cp = remote(rows_in.at[0, dz], rows_in.at[1, dz], c_s.at[dz], c_r.at[dz], sibling, tp)
        cp.start()
        c_copies.append(cp)

    forward(0)

    arrived(sg)
    arrived(su)
    hid = (silu(dot_t(nrm2, sg[...])) * dot_t(nrm2, su[...])).astype(BF16)
    arrived(sd)
    sh_copies = []
    for d in list(range(1, n_tp)) + [0]:
        peer = tp_peer(d)
        part = dot(hid, sd[:, pl.ds(pl.multiple_of(peer * feats, 128), feats)]).astype(BF16)
        sh_send[d] = part
        if d > 0:
            cp = remote(sh_send.at[d], sh_recv.at[d], sh_s.at[d], sh_r.at[d], ep, peer)
            cp.start()
            sh_copies.append(cp)

    lax.fori_loop(half, batch, update, 0)

    comb_copies, down_copies = [], []

    def expert_rows(r, lo):
        x = rows_in[r, lo : lo + span]
        x = x.reshape(span * batch, width + 128)
        return x[:, :width], x[:, width:].astype(F32)

    for ch in range(chunks):
        lo = ch * span
        for dz in range(max(lo, 1), lo + span):
            forward(dz)
        if ch == 0:
            arrived(eg)
            arrived(eu)
            arrived(ed)
        for dz in range(lo, lo + span):
            c_copies[dz].wait_recv()
        x1, w1 = expert_rows(1, lo)
        x0, w0 = expert_rows(0, lo)
        x = jnp.concatenate([x1, x0], axis=0)
        w = jnp.concatenate([w1, w0], axis=0)
        lane_id = lax.broadcasted_iota(jnp.int32, w.shape, 1)
        mine = (lane_id == ep) | (lane_id == ep + n_ep)
        share = jnp.sum(jnp.where(mine, w, 0.0), axis=1, keepdims=True)
        hidden = (silu(dot_t(x, eg[...])) * dot_t(x, eu[...]) * share).astype(BF16)
        comb_send[ch] = dot(hidden[: span * batch], ed[...]).astype(BF16)
        cp = remote(comb_send.at[ch], comb_recv.at[ch], cb_s.at[ch], cb_r.at[ch], sibling, tp)
        cp.start()
        comb_copies.append(cp)
        kept[...] = dot(hidden[span * batch :], ed[...])
        cp.wait_recv()
        for d in list(range(1, n_tp)) + [0]:
            peer = tp_peer(d)
            cols = pl.ds(pl.multiple_of(peer * feats, 128), feats)
            down_send[ch, d] = (kept[:, cols] + comb_recv[ch, :, cols].astype(F32)).astype(BF16)
            if d > 0:
                cp = remote(
                    down_send.at[ch, d], down_recv.at[ch, d],
                    dn_s.at[ch, d], dn_r.at[ch, d], ep, peer,
                )
                cp.start()
                down_copies.append(cp)

    back_copies = []
    for ch in range(chunks):
        summed = down_send[ch, 0].astype(F32)
        for d in range(1, n_tp):
            down_copies[ch * (n_tp - 1) + d - 1].wait_recv()
            summed = summed + down_recv[ch, d].astype(F32)
        back_send[ch * span : (ch + 1) * span] = summed.astype(BF16).reshape(span, batch, feats)
        for dz in range(max(ch * span, 1), (ch + 1) * span):
            cp = remote(
                back_send.at[dz], back_recv.at[dz], bk_s.at[dz], bk_r.at[dz], along_z(-dz), tp
            )
            cp.start()
            back_copies.append(cp)

    shared = sh_send[0].astype(F32)
    for d in range(1, n_tp):
        sh_copies[d - 1].wait_recv()
        shared = shared + sh_recv[d].astype(F32)
    result = shared + second[:, pl.ds(pl.multiple_of(tp * feats, 128), feats)].astype(F32)
    result = result + back_send[0].astype(F32)
    for dz in range(1, zs):
        back_copies[dz - 1].wait_recv()
        result = result + back_recv[dz].astype(F32)
    out[...] = result.astype(BF16)

    started = qk_copies + at_copies + z_copies + c_copies + sh_copies
    for cp in started + comb_copies + down_copies + back_copies:
        cp.wait_send()


def body(
    n_ep, n_tp,
    tokens, old_state, first_gain, query_weight, key_weight, value_weight, outgate_weight,
    lowrank_weight, decay_weight, decay_bias, head_gain, output_weight, second_gain,
    expert_gate, expert_up, expert_down, shared_gate, shared_up, shared_down,
    route_ids, route_weights,
):
    batch, width = tokens.shape
    key_width, value_count = old_state.shape[1], old_state.shape[2]
    heads = decay_weight.shape[1] // key_width
    feats = width // n_tp
    qk_cols = heads * key_width
    zs = n_ep // 2
    chunks = 2 if zs % 2 == 0 else 1
    rows = zs * batch // chunks
    vmem = pl.BlockSpec(memory_space=pltpu.VMEM)
    hbm = pl.BlockSpec(memory_space=pltpu.HBM)
    dma = pltpu.SemaphoreType.DMA
    big = [
        query_weight, key_weight, value_weight, outgate_weight, output_weight,
        expert_gate[0].T, expert_up[0].T, expert_down[0], shared_gate.T, shared_up.T, shared_down,
    ]
    scratch = [pltpu.VMEM(w.shape, BF16) for w in big]
    scratch += [
        dma((12,)),
        pltpu.VMEM((128, 128), F32),
        pltpu.VMEM((batch, width), BF16),
        pltpu.VMEM((batch, 2 * qk_cols), BF16),
        pltpu.VMEM((n_tp, batch, 2 * key_width), BF16),
        pltpu.VMEM((n_tp, batch, 2 * key_width), BF16),
        pltpu.VMEM((batch, value_count), F32),
        pltpu.VMEM((key_width, 128), F32),
        pltpu.VMEM((batch, width), BF16),
        pltpu.VMEM((n_tp, batch, width), BF16),
        pltpu.VMEM((batch, 128), F32),
        pltpu.VMEM((n_tp, batch, 128), F32),
        pltpu.VMEM((batch, width), BF16),
        pltpu.VMEM((2, zs, batch, width + 128), BF16),
        pltpu.VMEM((rows, width), F32),
        pltpu.VMEM((chunks, rows, width), BF16),
        pltpu.VMEM((chunks, rows, width), BF16),
        pltpu.VMEM((chunks, n_tp, rows, feats), BF16),
        pltpu.VMEM((chunks, n_tp, rows, feats), BF16),
        pltpu.VMEM((n_tp, batch, feats), BF16),
        pltpu.VMEM((n_tp, batch, feats), BF16),
        pltpu.VMEM((zs, batch, feats), BF16),
        pltpu.VMEM((zs, batch, feats), BF16),
    ]
    counts = ((n_tp,), (n_tp,), (n_tp,), (zs,), (zs,), (chunks,), (chunks, n_tp), (n_tp,), (zs,))
    for count in counts:
        scratch += [dma(count), dma(count)]
    layer_out, new_state = pl.pallas_call(
        functools.partial(layer_kernel, n_ep, n_tp, heads),
        out_shape=(
            jax.ShapeDtypeStruct((batch, feats), BF16),
            pltpu.VMEM(old_state.shape, BF16),
        ),
        in_specs=[vmem] * 9 + [hbm] * 12,
        out_specs=(vmem, vmem),
        scratch_shapes=scratch,
        compiler_params=pltpu.CompilerParams(
            collective_id=0, has_side_effects=True, vmem_limit_bytes=57 * 1024 * 1024
        ),
    )(
        tokens, first_gain.reshape(-1, 128), lowrank_weight.T, decay_weight, decay_bias[None],
        head_gain.reshape(-1, 128), second_gain.reshape(-1, 128), route_ids.T, route_weights.T,
        old_state, query_weight, key_weight, value_weight, outgate_weight, output_weight,
        expert_gate.swapaxes(1, 2), expert_up.swapaxes(1, 2), expert_down,
        shared_gate.T, shared_up.T, shared_down,
    )
    return layer_out, new_state


def solution(mesh):
    placed = (
        P("ep", None),
        P("ep", None, "tp"),
        P(),
        P("tp", None),
        P("tp", None),
        P(None, "tp"),
        P(None, "tp"),
        P(),
        P(),
        P(),
        P("tp"),
        P("tp", None),
        P(),
        P("ep", None, "tp"),
        P("ep", None, "tp"),
        P("ep", "tp", None),
        P(None, "tp"),
        P(None, "tp"),
        P("tp", None),
        P("ep", None),
        P("ep", None),
    )
    return jax.shard_map(
        functools.partial(body, mesh.shape["ep"], mesh.shape["tp"]),
        mesh=mesh,
        in_specs=placed,
        out_specs=(P("ep", "tp"), P("ep", None, "tp")),
        check_vma=False,
    )
```
